128 devices in a mesh: sp: 16 (over z, x), dp: 8 (over y, core).
Axes of the slice: x: 4, y: 4, z: 4, core: 2. Of those that a mesh axis runs over, the one named last changes fastest.
Arguments:
- hidden_in: bfloat16 [8, 2048, 2048], P('dp', 'sp'), may hold values from -6 to 6
- in_weight: bfloat16 [2048, 512], P(('sp', 'dp')), may hold values from -0.125 to 0.125
- lam_real: float32 [32, 64], replicated, may hold values from -4 to 0, as said below
- lam_imag: float32 [32, 64], replicated, may hold values from 1 to 200
- log_step: float32 [32], replicated, may hold values from -4.61 to -2.3
- b_real: float32 [32, 64, 16], replicated, may hold values from -1 to 1
- b_imag: float32 [32, 64, 16], replicated, may hold values from -1 to 1
- c_real: float32 [32, 16, 64], replicated, may hold values from -0.3 to 0.3
- c_imag: float32 [32, 16, 64], replicated, may hold values from -0.3 to 0.3
- skip_weight: float32 [512], replicated, may hold values from -4 to 4
- lin_weight: bfloat16 [512, 2048], P(None, ('sp', 'dp')), may hold values from -0.25 to 0.25
- gate_weight: bfloat16 [512, 2048], P(None, ('sp', 'dp')), may hold values from -0.25 to 0.25
Outputs:
- mixed: bfloat16 [8, 2048, 2048], P('dp', 'sp')
The draws below stay inside these ranges and needn't reach their ends.
Inputs may be any that keep to these rules, and one draw needn't show every extreme that they name: `lam_real`: negative in every entry.
All inputs are finite; a program needn't handle non-finite values.
Results may differ from the reference program's by a relative error of at most 0.0047.
The reference program's roundings to bfloat16 on the way (of `inputs` and `mixer_out`) count: a program that leaves them out, or rounds other values in their place, can miss the bound.
Values may be sent and summed in bfloat16 or wider, within the bound.
A program may use at most 64 MiB of HBM per device.

```python
import math
import jax
import jax.numpy as jnp
from jax import lax

D = 2048
GROUPS = 32
CH_GROUP = 16
STATES = 64
U = 512
LEN = 2048
BATCH = 8


def decay_plan(key):
    base = jax.random.fold_in(key, 11)
    first, second, third, fourth = jax.random.split(base, 4)
    log_step = jax.random.uniform(first, (GROUPS,), jnp.float32, math.log(0.01), math.log(0.1))
    share = 0.5
    quick = jax.random.uniform(second, (GROUPS,), jnp.float32) < share
    quick_rate = jnp.exp(jax.random.uniform(third, (GROUPS, STATES), jnp.float32, math.log(1.0 / 100.0), math.log(1.0 / 30.0)))
    slow_rate = jnp.exp(jax.random.uniform(fourth, (GROUPS, STATES), jnp.float32, math.log(0.2 / LEN), math.log(2.0 / LEN)))
    rate = jnp.where(quick[:, None], quick_rate, slow_rate)
    lam_real = -rate / jnp.exp(log_step)[:, None]
    return (lam_real, log_step)


def draw_lam_real(key, part):
    return decay_plan(key)[0]


def draw_log_step(key, part):
    return decay_plan(key)[1]


def shard_levels(key, dims, cuts, low, largest):
    def one(dim, parts):
        steps = jax.random.uniform(jax.random.fold_in(jax.random.fold_in(key, 6), dim), (parts,), jnp.float32, low / len(cuts), largest / len(cuts))
        return jnp.repeat(jnp.exp(steps), dims[dim] // parts).reshape((-1,) + (1,) * (len(dims) - dim - 1))

    factor_of = one(*cuts[0])
    for cut in cuts[1:]:
        factor_of = factor_of * one(*cut)
    return factor_of


def noise(key, extent, spread, reach, cuts=(), kind=jnp.bfloat16):
    drawn = jax.random.normal(key, extent, jnp.float32) * spread
    if len(cuts) > 0:
        drawn = shard_levels(key, extent, cuts, -0.22, 0.18) * drawn
    return jnp.clip(drawn, min=-reach, max=reach).astype(kind)


def setup_inputs(seed: int = 0) -> dict:
    key_of = jax.random.split(jax.random.key(seed), 13)
    return {
        "hidden_in": noise(key_of[0], (BATCH, LEN, D), 1.0, 6.0, ((0, 8), (1, 16))),
        "in_weight": noise(key_of[1], (D, U), D ** -0.5, 0.125, ((0, 128),)),
        "lam_real": draw_lam_real(jax.random.fold_in(key_of[12], 71), 0),
        "lam_imag": jnp.clip(jax.random.uniform(key_of[3], (GROUPS, STATES), jnp.float32, 1.0, 200.0), 1.0, 200.0),
        "log_step": draw_log_step(jax.random.fold_in(key_of[12], 71), 0),
        "b_real": noise(key_of[5], (GROUPS, STATES, CH_GROUP), (2 * CH_GROUP) ** -0.5, 1.0, (), jnp.float32),
        "b_imag": noise(key_of[6], (GROUPS, STATES, CH_GROUP), (2 * CH_GROUP) ** -0.5, 1.0, (), jnp.float32),
        "c_real": noise(key_of[7], (GROUPS, CH_GROUP, STATES), 0.05, 0.3, (), jnp.float32),
        "c_imag": noise(key_of[8], (GROUPS, CH_GROUP, STATES), 0.05, 0.3, (), jnp.float32),
        "skip_weight": noise(key_of[9], (U,), 1.0, 4.0, (), jnp.float32),
        "lin_weight": noise(key_of[10], (U, D), U ** -0.5, 0.25, ((1, 128),)),
        "gate_weight": noise(key_of[11], (U, D), U ** -0.5, 0.25, ((1, 128),)),
    }


def step_factors(lam_real, lam_imag, log_step, b_real, b_imag):
    step = jnp.exp(log_step)[:, None]
    xpart = lam_real * step
    wpart = lam_imag * step
    decay_re = jnp.exp(xpart) * jnp.cos(wpart)
    decay_im = jnp.exp(xpart) * jnp.sin(wpart)
    numer_re = jnp.expm1(xpart) * jnp.cos(wpart) - 2.0 * jnp.sin(0.5 * wpart) ** 2
    numer_im = decay_im
    magnitude = lam_real * lam_real + lam_imag * lam_imag
    ratio_re = (numer_re * lam_real + numer_im * lam_imag) / magnitude
    ratio_im = (numer_im * lam_real - numer_re * lam_imag) / magnitude
    bbar_re = ratio_re[..., None] * b_real - ratio_im[..., None] * b_imag
    bbar_im = ratio_re[..., None] * b_imag + ratio_im[..., None] * b_real
    return decay_re, decay_im, bbar_re, bbar_im


def combine(left, right):
    lre, lim, lbre, lbim = left
    rre, rim, rbre, rbim = right
    return (rre * lre - rim * lim, rre * lim + rim * lre,
            rre * lbre - rim * lbim + rbre, rre * lbim + rim * lbre + rbim)


def reference(hidden_in, in_weight, lam_real, lam_imag, log_step, b_real, b_imag, c_real, c_imag, skip_weight, lin_weight, gate_weight):
    highest = lax.Precision.HIGHEST
    flat = hidden_in.reshape(BATCH * LEN, D)
    inputs = jnp.dot(flat, in_weight, preferred_element_type=jnp.float32).astype(jnp.bfloat16)
    inputs = inputs.reshape(BATCH, LEN, U)
    decay_re, decay_im, bbar_re, bbar_im = step_factors(lam_real, lam_imag, log_step, b_real, b_imag)
    lanes = GROUPS * STATES
    flat_re = decay_re.reshape(lanes)
    flat_im = decay_im.reshape(lanes)
    block = math.gcd(LEN, 512)

    def one_sequence(sequence):
        blocks = sequence.reshape(LEN // block, block, U)

        def block_step(carry, piece):
            carry_re, carry_im = carry
            source = piece.astype(jnp.float32)
            shaped = source.reshape(block, GROUPS, CH_GROUP)
            drive_re = jnp.einsum('tgh,gph->tgp', shaped, bbar_re, precision=highest).reshape(block, lanes)
            drive_im = jnp.einsum('tgh,gph->tgp', shaped, bbar_im, precision=highest).reshape(block, lanes)
            are = jnp.broadcast_to(flat_re, drive_re.shape)
            aim = jnp.broadcast_to(flat_im, drive_re.shape)
            cum_re, cum_im, local_re, local_im = lax.associative_scan(combine, (are, aim, drive_re, drive_im), axis=0)
            state_re = local_re + cum_re * carry_re - cum_im * carry_im
            state_im = local_im + cum_re * carry_im + cum_im * carry_re
            summed = (jnp.einsum('tgp,ghp->tgh', state_re.reshape(block, GROUPS, STATES), c_real, precision=highest)
                      - jnp.einsum('tgp,ghp->tgh', state_im.reshape(block, GROUPS, STATES), c_imag, precision=highest))
            result = jax.nn.gelu(summed.reshape(block, U) + skip_weight * source)
            return (state_re[-1], state_im[-1]), result.astype(jnp.bfloat16)

        zeros = jnp.zeros((lanes,), jnp.float32)
        _, results = lax.scan(block_step, (zeros, zeros), blocks)
        return results.reshape(LEN, U)

    mixer_out = lax.map(one_sequence, inputs).reshape(BATCH * LEN, U)
    linear = jnp.dot(mixer_out, lin_weight, preferred_element_type=jnp.float32)
    gate = jnp.dot(mixer_out, gate_weight, preferred_element_type=jnp.float32)
    mixed = (linear * jax.nn.sigmoid(gate)).astype(jnp.bfloat16)
    return mixed.reshape(BATCH, LEN, D)
```

```python
import functools

import jax
import jax.numpy as jnp
from jax import lax
from jax.experimental import pallas as pl
from jax.experimental.pallas import tpu as pltpu
from jax.sharding import PartitionSpec as P

MESH = pl.DeviceIdType.MESH
ANY = pl.ANY
HIGH = lax.Precision.HIGHEST
NT = (((1,), (1,)), ((), ()))
F32, BF16 = jnp.float32, jnp.bfloat16

TOK = 128
GRP = 16
TILES = 8
STR = 136
SEQ = 2 * TILES * STR

ITEMS = (
    ("w", 0, 0, (2, 1, 0)),
    ("w", 1, 0, (2, 0, 1)),
    ("l", None, 0, (1, 0, 2)),
    ("l", None, 256, (0, 1, 2)),
    ("g", None, 0, (1, 2, 0)),
    ("g", None, 256, (0, 2, 1)),
)
PER_ITEM = 12


def split(a):
    high = a.astype(BF16)
    return high, (a - high.astype(F32)).astype(BF16)


def kernel(
    hid, win, lamr, lami, lst, br, bi, cr, ci, skip, lin, gate, out,
    hbuf, wbuf, lbuf, gbuf, drive, bh, bl, ch, cl, ubuf,
    lamv, lstv, bv, cv, skv, linv, gatev, fbuf, fsend, msend, mbuf, obuf,
    loc, rs, rr, hs, hr, ws, wr, fs, fr, ms, mr, ds_, dr_, os_,
):
    sp, dp = lax.axis_index("sp"), lax.axis_index("dp")
    z, x, y, h = lax.div(sp, 4), lax.rem(sp, 4), lax.div(dp, 2), lax.rem(dp, 2)
    at = (z, x, y)
    other = 1 - h
    peer = (sp, y * 2 + other)

    def device(pos):
        return (pos[0] * 4 + pos[1], pos[2] * 2 + h)

    def moved(axis, by):
        pos = list(at)
        pos[axis] = lax.rem(at[axis] + by + 4, 4)
        return device(pos)

    def remote(src, dst, send, recv, to):
        return pltpu.make_async_remote_copy(
            src_ref=src, dst_ref=dst, send_sem=send, recv_sem=recv, device_id=to, device_id_type=MESH
        )

    half_rows = pl.ds(h * GRP, GRP)
    half_cols = pl.ds(pl.multiple_of(h * 256, 256), 256)
    other_cols = pl.ds(pl.multiple_of(other * 256, 256), 256)
    loads = [
        (win.at[:, half_cols], wbuf.at[z, x, y, h]),
        (lin, linv),
        (gate, gatev),
        (hid.at[0], hbuf.at[h]),
        (lamr.at[half_rows], lamv.at[0]),
        (lami.at[half_rows], lamv.at[1]),
        (br.at[half_rows], bv.at[0]),
        (bi.at[half_rows], bv.at[1]),
        (cr.at[half_rows], cv.at[0]),
        (ci.at[half_rows], cv.at[1]),
        (skip.at[:, half_cols], skv),
        (lst, lstv),
    ]
    loads = [pltpu.make_async_copy(s, d, loc.at[k]) for k, (s, d) in enumerate(loads)]
    for c in loads:
        c.start()

    barrier = pltpu.get_barrier_semaphore()
    pl.semaphore_signal(barrier, inc=1, device_id=peer, device_id_type=MESH)
    for k in range(1, 4):
        pl.semaphore_signal(barrier, inc=1, device_id=moved(2, k), device_id_type=MESH)
    for k in range(1, 16):
        pl.semaphore_signal(barrier, inc=1, device_id=(lax.rem(sp + k, 16), dp), device_id_type=MESH)
    pl.semaphore_wait(barrier, 19)

    w_pair = remote(win.at[:, other_cols], wbuf.at[z, x, y, h], ws, wr, peer)
    w_pair.start()
    h_pair = remote(hid.at[0], hbuf.at[h], hs, hr, peer)
    h_pair.start()

    bufs = {"w": wbuf, "l": lbuf, "g": gbuf}

    def slab(item, phase, i, cols=None):
        name, core, first, order = ITEMS[item]
        idx = [at[a] for a in range(3)]
        for a in order[: phase - 1]:
            idx[a] = slice(None)
        idx[order[phase - 1]] = i
        start, width = cols if cols is not None else (0, 256)
        return bufs[name].at[
            idx[0], idx[1], idx[2], h if core is None else core, :, pl.ds(first + start, width)
        ]

    def turn(axis, by):
        return lax.rem(at[axis] + by + 4, 4)

    def direct(item, phase):
        axis = ITEMS[item][3][phase - 1]
        copies = []
        for k in range(1, 4):
            sem = item * PER_ITEM + (phase - 1) * 3 + k - 1
            own = slab(item, phase, at[axis])
            copies.append(remote(own, own, rs.at[sem], rr.at[sem], moved(axis, k)))
        return copies

    H0, H1 = (0, 128), (128, 128)

    def last(item):
        axis = ITEMS[item][3][2]
        sem = item * PER_ITEM + 6
        plan = (
            (0, H0, 1), (0, H1, -1), (0, H1, 1), (0, H0, -1), (-1, H0, 1), (1, H1, -1),
        )
        copies = []
        for k, (which, cols, by) in enumerate(plan):
            piece = slab(item, 3, turn(axis, which), cols)
            copies.append(remote(piece, piece, rs.at[sem + k], rr.at[sem + k], moved(axis, by)))
        return copies

    first, second, third = {}, {}, {}
    for i in range(6):
        first[i], second[i], third[i] = direct(i, 1), direct(i, 2), last(i)

    passed = {}

    def pass_on(item, which):
        axis = ITEMS[item][3][2]
        piece = slab(item, 3, turn(axis, which))
        sem = (item - 2) * 4 + which + 1
        passed[sem] = remote(piece, piece, ds_.at[sem], dr_.at[sem], peer)
        passed[sem].start()

    def start(copies):
        for c in copies:
            c.start()

    def arrived(copies):
        for c in copies:
            c.wait_recv()

    loads[0].wait()
    w_pair.wait_recv()
    start(first[0])
    start(first[1])

    eye = (
        lax.broadcasted_iota(jnp.int32, (16, 16), 0) == lax.broadcasted_iota(jnp.int32, (16, 16), 1)
    ).astype(F32)
    for k, (stage, buf) in enumerate(((linv, lbuf), (gatev, gbuf))):
        loads[1 + k].wait()
        turned = lax.dot_general(eye.astype(BF16), stage[...], NT, preferred_element_type=F32)
        buf[z, x, y, h] = turned.astype(BF16)
    for i in range(2, 6):
        start(first[i])

    for c in loads[4:]:
        c.wait()
    row8 = lax.broadcasted_iota(jnp.int32, (8, 128), 0)
    lane8 = lax.broadcasted_iota(jnp.int32, (8, 128), 1)
    log_step = jnp.zeros((8, 128), F32)
    for g in range(GRP):
        here = (row8 == g // 2) & ((lane8 >= 64) == (g % 2 == 1))
        log_step = jnp.where(here, lstv[h * GRP + g], log_step)

    def pairs(k):
        both = [lamv[k, pl.ds(q, 8, stride=2), :] for q in range(2)]
        return jnp.concatenate(both, axis=1)

    lam_re, lam_im = pairs(0), pairs(1)
    step = jnp.exp(log_step)
    xpart = lam_re * step
    wpart = lam_im * step
    ex = jnp.exp(xpart)
    cosw, sinw, sinh_ = jnp.cos(wpart), jnp.sin(wpart), jnp.sin(0.5 * wpart)
    a_re, a_im = ex * cosw, ex * sinw
    plain = ex == 1.0
    em1 = jnp.where(plain, xpart, (ex - 1.0) * xpart / jnp.log(jnp.where(plain, 2.0, ex)))
    num_re = em1 * cosw - 2.0 * sinh_ * sinh_
    size = lam_re * lam_re + lam_im * lam_im
    ratio_re = (num_re * lam_re + a_im * lam_im) / size
    ratio_im = (a_im * lam_re - num_re * lam_im) / size
    p_re, p_im = a_re, a_im
    for _ in range(7):
        p_re, p_im = p_re * p_re - p_im * p_im, 2.0 * p_re * p_im

    for i in (0, 1):
        arrived(first[i])
        start(second[i])

    turned = [
        lax.dot_general(eye, bv[k].reshape(GRP * 64, 16), NT, precision=HIGH, preferred_element_type=F32)
        for k in range(2)
    ]
    low = lax.broadcasted_iota(jnp.int32, (16, 128), 1) < 64
    bh[...] = jnp.zeros_like(bh)
    bl[...] = jnp.zeros_like(bl)
    for j in range(TILES):
        b_re, b_im = (t[:, 128 * j : 128 * j + 128] for t in turned)
        r_re, r_im = ratio_re[j : j + 1], ratio_im[j : j + 1]
        for k, part in enumerate((r_re * b_re - r_im * b_im, r_re * b_im + r_im * b_re)):
            block = jnp.concatenate([jnp.where(low, part, 0.0), jnp.where(low, 0.0, part)], axis=0)
            rows = slice(32 * (j % 4), 32 * (j % 4) + 32)
            bh[j, rows, 128 * k : 128 * k + 128], bl[j, rows, 128 * k : 128 * k + 128] = split(block)

    for i in (0, 1):
        arrived(second[i])
        start(third[i][:4])
    for i in (4, 5, 2, 3):
        arrived(first[i])
        start(second[i])

    rows_c = lax.broadcasted_iota(jnp.int32, (128, 128), 0)
    lanes_c = lax.broadcasted_iota(jnp.int32, (128, 128), 1)
    same = lax.rem(lax.div(rows_c, 16), 2) == lax.div(lanes_c, 64)
    pair_of = lax.div(rows_c, 32)
    for a in range(2):
        for k, sign in ((0, 1.0), (1, -1.0)):
            c = cv[k, 8 * a : 8 * a + 8].reshape(128, 64) * sign
            c = jnp.where(same, jnp.concatenate([c, c], axis=1), 0.0)
            for j in range(4):
                cols = slice(256 * j + 128 * k, 256 * j + 128 * k + 128)
                ch[a, :, cols], cl[a, :, cols] = split(jnp.where(pair_of == j, c, 0.0))

    for k in (0, 1):
        for i in (0, 1):
            third[i][k].wait_recv()
            third[i][4 + k].start()
    for i in (4, 5):
        arrived(second[i])
        start(third[i][:4])
        pass_on(i, 0)
    for i in (0, 1):
        arrived(third[i][2:])
    for i in (2, 3):
        arrived(second[i])
        start(third[i][:4])
        pass_on(i, 0)

    loads[3].wait()
    h_pair.wait_recv()
    u = jnp.dot(
        hbuf[...].reshape(2 * TOK, 2048), wbuf[...].reshape(2048, 256), preferred_element_type=F32
    ).astype(BF16)
    ubuf[...] = u
    for j in range(TILES):
        cols = u[:, 128 * (j // 4) : 128 * (j // 4) + 128]
        d = jnp.dot(cols, bh[j], preferred_element_type=F32)
        d += jnp.dot(cols, bl[j], preferred_element_type=F32)
        for s in range(2):
            for k in range(2):
                rows = pl.ds(s * SEQ + (k * TILES + j) * STR, TOK)
                drive[rows, :] = d[TOK * s : TOK * s + TOK, 128 * k : 128 * k + 128]

    def scan(init, keep):
        def body(i, carry):
            carry = list(carry)
            for n in range(8):
                t = i * 8 + n
                for s in range(2):
                    at_re = pl.ds(s * SEQ + t, TILES, stride=STR)
                    at_im = pl.ds(s * SEQ + TILES * STR + t, TILES, stride=STR)
                    re, im = carry[2 * s], carry[2 * s + 1]
                    carry[2 * s] = a_re * re - a_im * im + drive[at_re, :]
                    carry[2 * s + 1] = a_re * im + a_im * re + drive[at_im, :]
                    if keep:
                        drive[at_re, :] = carry[2 * s]
                        drive[at_im, :] = carry[2 * s + 1]
            return tuple(carry)

        return lax.fori_loop(0, TOK // 8, body, init)

    zero = jnp.zeros((8, 128), F32)
    ends = scan((zero,) * 4, False)
    for k in range(4):
        fsend[k] = ends[k]

    def to_later(k):
        return remote(fsend, fbuf.at[sp], fs.at[k], fr.at[sp], (lax.rem(sp + k, 16), dp))

    for k in range(1, 16):

        @pl.when(sp + k < 16)
        def _():
            to_later(k).start()

    for i in (4, 5, 2, 3):
        for k in (0, 1):
            third[i][k].wait_recv()
            third[i][4 + k].start()
    for i in (4, 5, 2, 3):
        arrived(third[i][2:4])
        pass_on(i, -1)
        pass_on(i, 1)

    def fold(j, carry):
        remote(fsend, fbuf.at[j], fs.at[0], fr.at[j], peer).wait_recv()
        new = []
        for s in range(2):
            re, im = carry[2 * s], carry[2 * s + 1]
            new.append(p_re * re - p_im * im + fbuf[j, 2 * s])
            new.append(p_re * im + p_im * re + fbuf[j, 2 * s + 1])
        return tuple(new)

    scan(lax.fori_loop(0, sp, fold, (zero,) * 4), True)

    for a in range(2):
        tiles = []
        for j in range(4):
            for k in range(2):
                rows = [pl.ds(s * SEQ + (k * TILES + 4 * a + j) * STR, TOK) for s in range(2)]
                tiles.append(jnp.concatenate([drive[r, :] for r in rows], axis=0))
        s_high, s_low = split(jnp.concatenate(tiles, axis=1))
        summed = lax.dot_general(s_high, ch[a], NT, preferred_element_type=F32)
        summed += lax.dot_general(s_low, ch[a], NT, preferred_element_type=F32)
        summed += lax.dot_general(s_high, cl[a], NT, preferred_element_type=F32)
        cols = slice(128 * a, 128 * a + 128)
        mixer = jax.nn.gelu(summed + skv[:, cols] * ubuf[:, cols].astype(F32)).astype(BF16)
        mine = jnp.where(h == 0, mixer[:TOK].astype(F32), mixer[TOK:].astype(F32)).astype(BF16)
        theirs = jnp.where(h == 0, mixer[TOK:].astype(F32), mixer[:TOK].astype(F32)).astype(BF16)
        mbuf[h, :, cols] = mine
        msend[:, cols] = theirs
    m_pair = remote(msend, mbuf.at[h], ms, mr, peer)
    m_pair.start()

    for i in (4, 5, 2, 3):
        arrived(third[i][4:])
        pass_on(i, 2)
    m_pair.wait_recv()
    for sem in sorted(passed):
        passed[sem].wait_recv()

    m = jnp.concatenate([mbuf[0], mbuf[1]], axis=1)
    puts = []
    for n in range(8):
        rows = (n // 2, slice(2 * (n % 2), 2 * (n % 2) + 2))
        linear = lax.dot_general(m, lbuf[rows].reshape(256, 512), NT, preferred_element_type=F32)
        gated = lax.dot_general(m, gbuf[rows].reshape(256, 512), NT, preferred_element_type=F32)
        cols = slice(256 * n, 256 * n + 256)
        obuf[:, cols] = (linear * jax.nn.sigmoid(gated)).astype(BF16)
        puts.append(
            pltpu.make_async_copy(obuf.at[:, pl.ds(256 * n, 256)], out.at[0, :, pl.ds(256 * n, 256)], os_.at[n])
        )
        puts[-1].start()

    for i in range(6):
        for c in first[i] + second[i] + third[i]:
            c.wait_send()
    for sem in sorted(passed):
        passed[sem].wait_send()
    for c in (w_pair, h_pair, m_pair):
        c.wait_send()
    for k in range(1, 16):

        @pl.when(sp + k < 16)
        def _():
            to_later(k).wait_send()

    for c in puts:
        c.wait()


def shards(hid, win, lamr, lami, lst, br, bi, cr, ci, skip, lin, gate):
    dma = pltpu.SemaphoreType.DMA
    vmem = pltpu.VMEM
    return pl.pallas_call(
        kernel,
        name="mixer",
        out_shape=jax.ShapeDtypeStruct((1, TOK, 2048), BF16),
        in_specs=[pl.BlockSpec(memory_space=ANY)] * 12,
        out_specs=pl.BlockSpec(memory_space=ANY),
        scratch_shapes=[
            vmem((2, TOK, 2048), BF16),
            vmem((4, 4, 4, 2, 16, 256), BF16),
            vmem((4, 4, 4, 2, 16, 512), BF16),
            vmem((4, 4, 4, 2, 16, 512), BF16),
            vmem((2 * SEQ, 128), F32),
            vmem((TILES, 128, 256), BF16),
            vmem((TILES, 128, 256), BF16),
            vmem((2, 128, 1024), BF16),
            vmem((2, 128, 1024), BF16),
            vmem((2 * TOK, 256), BF16),
            vmem((2, GRP, 64), F32),
            pltpu.SMEM((32,), F32),
            vmem((2, GRP, 64, 16), F32),
            vmem((2, GRP, 16, 64), F32),
            vmem((1, 256), F32),
            vmem((512, 16), BF16),
            vmem((512, 16), BF16),
            vmem((16, 4, 8, 128), F32),
            vmem((4, 8, 128), F32),
            vmem((TOK, 256), BF16),
            vmem((2, TOK, 256), BF16),
            vmem((TOK, 2048), BF16),
            dma((12,)),
            dma((6 * PER_ITEM,)),
            dma((6 * PER_ITEM,)),
            dma, dma, dma, dma,
            dma((16,)),
            dma((16,)),
            dma, dma,
            dma((16,)),
            dma((16,)),
            dma((8,)),
        ],
        compiler_params=pltpu.CompilerParams(
            collective_id=0, has_side_effects=True, vmem_limit_bytes=48 * 1024 * 1024
        ),
    )(hid, win, lamr, lami, lst, br, bi, cr, ci, skip.reshape(1, 512), lin, gate)


def solution(mesh):
    placed = (
        P("dp", "sp", None),
        P(("sp", "dp"), None),
        *(P(),) * 8,
        P(None, ("sp", "dp")),
        P(None, ("sp", "dp")),
    )
    return jax.shard_map(
        shards, mesh=mesh, in_specs=placed, out_specs=P("dp", "sp", None), check_vma=False
    )
```

```python
import functools

import jax
import jax.numpy as jnp
from jax import lax
from jax.experimental import pallas as pl
from jax.experimental.pallas import tpu as pltpu
from jax.sharding import PartitionSpec as P

MESH = pl.DeviceIdType.MESH
ANY = pl.ANY
HIGH = lax.Precision.HIGHEST
NT = (((1,), (1,)), ((), ()))
F32, BF16 = jnp.float32, jnp.bfloat16

TOK = 128
GRP = 16
TILES = 8
STR = 136
SEQ = 2 * TILES * STR

ITEMS = ((0, (1, 2, 0)), (256, (0, 2, 1)))
PER_ITEM = 12


def split(a):
    high = a.astype(BF16)
    return high, (a - high.astype(F32)).astype(BF16)


def kernel(
    hid, win, lamr, lami, lst, br, bi, cr, ci, skip, lin, gate, out,
    hbuf, wbuf, lbuf, gbuf, drive, bh, bl, ch, cl, ubuf,
    lamv, lstv, bv, cv, skv, wsend, fact, fbuf, fsend, msend, mbuf,
    loc, rs, rr, hs, hr, ws, wr, ls, lr, fs, fr, ms, mr, ds_, dr_,
):
    scopes = []

    def phase(name):
        if scopes:
            scopes.pop().__exit__(None, None, None)
        if name:
            scopes.append(jax.named_scope(name))
            scopes[-1].__enter__()

    phase("loads")
    sp, dp = lax.axis_index("sp"), lax.axis_index("dp")
    z, x, y, h = lax.div(sp, 4), lax.rem(sp, 4), lax.div(dp, 2), lax.rem(dp, 2)
    at = (z, x, y)
    other = 1 - h
    peer = (sp, y * 2 + other)

    def device(pos):
        return (pos[0] * 4 + pos[1], pos[2] * 2 + h)

    def moved(axis, by):
        pos = list(at)
        pos[axis] = lax.rem(at[axis] + by + 4, 4)
        return device(pos)

    def remote(src, dst, send, recv, to):
        return pltpu.make_async_remote_copy(
            src_ref=src, dst_ref=dst, send_sem=send, recv_sem=recv, device_id=to, device_id_type=MESH
        )

    half_rows = pl.ds(h * GRP, GRP)
    half_cols = pl.ds(pl.multiple_of(h * 256, 256), 256)
    other_cols = pl.ds(pl.multiple_of(other * 256, 256), 256)
    loads = [
        (win.at[:, half_cols], wbuf.at[z, x, y, h]),
        (win.at[:, other_cols], wsend),
        (lin, lbuf.at[z, x, y, h]),
        (gate, gbuf.at[z, x, y, h]),
        (hid.at[0], hbuf.at[h]),
        (lamr.at[half_rows], lamv.at[0]),
        (lami.at[half_rows], lamv.at[1]),
        (br.at[half_rows], bv.at[0]),
        (bi.at[half_rows], bv.at[1]),
        (cr.at[half_rows], cv.at[0]),
        (ci.at[half_rows], cv.at[1]),
        (skip.at[:, half_cols], skv),
        (lst, lstv),
    ]
    loads = [pltpu.make_async_copy(s, d, loc.at[k]) for k, (s, d) in enumerate(loads)]
    for c in loads:
        c.start()

    phase("barrier")
    def place(dz, dx, dy, core):
        return (
            lax.rem(z + dz, 4) * 4 + lax.rem(x + dx, 4),
            lax.rem(y + dy, 4) * 2 + core,
        )

    def in_plane(i, j, core):
        return place(h * i, other * i, j, core)

    senders = [place(0, i, j, 0) for i in range(4) for j in range(4)]
    senders += [place(i, 0, j, 1) for i in range(4) for j in range(4)]
    senders += [
        place(other * i + h * j, other * j + h * i, 0, h) for i in range(1, 4) for j in range(4)
    ]
    barrier = pltpu.get_barrier_semaphore()
    for to in senders:
        pl.semaphore_signal(barrier, inc=1, device_id=to, device_id_type=MESH)
    pl.semaphore_wait(barrier, len(senders))

    def slab(item, phase, i, cols=None):
        first, order = ITEMS[item]
        idx = [at[a] for a in range(3)]
        for a in order[: phase - 1]:
            idx[a] = slice(None)
        idx[order[phase - 1]] = i
        start, width = cols if cols is not None else (0, 256)
        return gbuf.at[idx[0], idx[1], idx[2], h, :, pl.ds(first + start, width)]

    def turn(axis, by):
        return lax.rem(at[axis] + by + 4, 4)

    def direct(item, phase):
        axis = ITEMS[item][1][phase - 1]
        copies = []
        for k in range(1, 4):
            sem = item * PER_ITEM + (phase - 1) * 3 + k - 1
            own = slab(item, phase, at[axis])
            copies.append(remote(own, own, rs.at[sem], rr.at[sem], moved(axis, k)))
        return copies

    H0, H1 = (0, 128), (128, 128)

    def last(item):
        axis = ITEMS[item][1][2]
        sem = item * PER_ITEM + 6
        plan = (
            (0, H0, 1), (0, H1, -1), (0, H1, 1), (0, H0, -1), (-1, H0, 1), (1, H1, -1),
        )
        copies = []
        for k, (which, cols, by) in enumerate(plan):
            piece = slab(item, 3, turn(axis, which), cols)
            copies.append(remote(piece, piece, rs.at[sem + k], rr.at[sem + k], moved(axis, by)))
        return copies

    first, second, third = {}, {}, {}
    for i in range(2):
        first[i], second[i], third[i] = direct(i, 1), direct(i, 2), last(i)

    passed = {}

    def pass_on(piece):
        sem = len(passed)
        passed[sem] = remote(piece, piece, ds_.at[sem], dr_.at[sem], peer)
        passed[sem].start()

    def pass_gate(item, which):
        pass_on(slab(item, 3, turn(ITEMS[item][1][2], which)))

    def pass_lin(which):
        pass_on(lbuf.at[:, :, turn(2, which), h])

    def start(copies):
        for c in copies:
            c.start()

    def arrived(copies):
        for c in copies:
            c.wait_recv()

    phase("first")
    loads[0].wait()
    loads[1].wait()
    own = wbuf.at[z, x, y, h]
    plane = []
    for j, i in sorted(((j, i) for j in range(4) for i in range(4)), key=lambda p: min(p[0], 1) + min(p[1], 1)):
        for core, src in ((h, own), (other, wsend)):
            if i + j > 0 or src is wsend:
                k = len(plane)
                slot = h * 16 + i * 4 + j
                plane.append(remote(src, own, ws.at[k], wr.at[slot], in_plane(i, j, core)))
                plane[-1].start()
    loads[2].wait()
    loads[3].wait()
    for i in range(2):
        start(first[i])
    lin_own = lbuf.at[z, x, y, h]
    lin_plane = [
        remote(lin_own, lin_own, ls.at[4 * i + j], lr.at[4 * i + j], place(i, j, 0, h))
        for i in range(4)
        for j in range(4)
        if i + j > 0
    ]
    start(lin_plane)
    loads[4].wait()
    h_pair = remote(hbuf.at[h], hbuf.at[h], hs, hr, peer)
    h_pair.start()

    def chunk(item, i, away):
        inner = lax.rem(at[1 - item] - i + 4, 4)
        final = lax.rem(at[item] + away + 4, 4)
        return wbuf.at[final, inner, :, item] if item == 0 else wbuf.at[inner, final, :, item]

    def to_neighbour(item, i, away, by, sem):
        piece = chunk(item, i, away)
        sem = item * PER_ITEM + sem
        return remote(piece, piece, rs.at[2 * PER_ITEM + sem], rr.at[2 * PER_ITEM + sem], moved(item, by))

    def lin_chunk(c, away, by, sem):
        piece = lbuf.at[:, :, turn(2, away), h, :, pl.ds(128 * c, 128)]
        return remote(piece, piece, ls.at[sem], lr.at[sem], moved(2, by))

    lin_up = [lin_chunk(c, 0, 1, 16 + c) for c in range(4)]
    lin_down = [lin_chunk(c, 0, -1, 20 + c) for c in range(4)]
    lin_far = [lin_chunk(c, -1, 1, 24 + c) for c in (0, 1)] + [lin_chunk(c, 1, -1, 24 + c) for c in (2, 3)]

    up = {(t, i): to_neighbour(t, i, 0, 1, i) for t in range(2) for i in range(4)}
    down = {(t, i): to_neighbour(t, i, 0, -1, 4 + i) for t in range(2) for i in range(4)}
    further = {(t, i): to_neighbour(t, i, -1, 1, 8 + i) for t in range(2) for i in (0, 1)}
    further.update({(t, i): to_neighbour(t, i, 1, -1, 8 + i) for t in range(2) for i in (3, 2)})

    def plane_arrived(item, i):
        for j in range(4):
            slot = item * 16 + i * 4 + j
            if i + j > 0:
                remote(own, own, ws.at[0], wr.at[slot], peer).wait_recv()

    phase("factors")
    for c in loads[5:]:
        c.wait()
    rows_g = lax.broadcasted_iota(jnp.int32, (GRP, 64), 0)
    log_step = jnp.zeros((GRP, 64), F32)
    for g in range(GRP):
        log_step = jnp.where(rows_g == g, lstv[h * GRP + g], log_step)
    lam_re, lam_im = lamv[0], lamv[1]
    step = jnp.exp(log_step)
    xpart = lam_re * step
    wpart = lam_im * step
    ex = jnp.exp(xpart)
    cosw, sinw, sinh_ = jnp.cos(wpart), jnp.sin(wpart), jnp.sin(0.5 * wpart)
    plain = ex == 1.0
    em1 = jnp.where(plain, xpart, (ex - 1.0) * xpart / jnp.log(jnp.where(plain, 2.0, ex)))
    num_re = em1 * cosw - 2.0 * sinh_ * sinh_
    num_im = ex * sinw
    size = lam_re * lam_re + lam_im * lam_im
    ratio_re = (num_re * lam_re + num_im * lam_im) / size
    ratio_im = (num_im * lam_re - num_re * lam_im) / size
    fact[0], fact[1] = ex * cosw, num_im

    def pairs(k):
        both = [fact[k, pl.ds(q, 8, stride=2), :] for q in range(2)]
        return jnp.concatenate(both, axis=1)

    a_re, a_im = pairs(0), pairs(1)
    p_re, p_im = a_re, a_im
    for _ in range(7):
        p_re, p_im = p_re * p_re - p_im * p_im, 2.0 * p_re * p_im

    phase("tables_b")
    rows_c = lax.broadcasted_iota(jnp.int32, (128, 128), 0)
    lanes_c = lax.broadcasted_iota(jnp.int32, (128, 128), 1)
    same = lax.rem(lax.div(rows_c, 16), 2) == lax.div(lanes_c, 64)
    pair_of = lax.div(rows_c, 32)

    def widened(part):
        part = part.reshape(128, 64)
        return jnp.where(same, jnp.concatenate([part, part], axis=1), 0.0)

    for a in range(2):
        groups = slice(8 * a, 8 * a + 8)
        r_re, r_im = ratio_re[groups].reshape(8, 1, 64), ratio_im[groups].reshape(8, 1, 64)
        b_re, b_im = bv[0, groups], bv[1, groups]
        for k, part in enumerate((r_re * b_re - r_im * b_im, r_re * b_im + r_im * b_re)):
            part = widened(part)
            for j in range(4):
                cols = slice(128 * k, 128 * k + 128)
                bh[4 * a + j, :, cols], bl[4 * a + j, :, cols] = split(jnp.where(pair_of == j, part, 0.0))

    phase("tables_c")
    for a in range(2):
        for k, sign in ((0, 1.0), (1, -1.0)):
            c = widened(cv[k, 8 * a : 8 * a + 8]) * sign
            for j in range(4):
                cols = slice(256 * j + 128 * k, 256 * j + 128 * k + 128)
                ch[a, :, cols], cl[a, :, cols] = split(jnp.where(pair_of == j, c, 0.0))

    phase("plane")
    remote(own, own, ws.at[0], wr.at[other * 16], peer).wait_recv()
    for i in (0, 1, 3, 2):
        for t in range(2):
            plane_arrived(t, i)
            up[t, i].start()
            down[t, i].start()
    phase("second")
    for i in range(2):
        arrived(first[i])
        start(second[i])
    phase("third_l")
    arrived(lin_plane)
    for c in range(4):
        lin_up[c].start()
        lin_down[(c + 2) % 4].start()
    pass_lin(0)
    phase("pass_w")
    for i in (0, 1, 3, 2):
        for t in range(2):
            (up if i in (0, 1) else down)[t, i].wait_recv()
            further[t, i].start()
    phase("third_g")
    for i in range(2):
        arrived(second[i])
        start(third[i][:2])
    for i in range(2):
        start(third[i][2:4])
        pass_gate(i, 0)
    phase("rest_w")
    for i in (0, 1, 3, 2):
        for t in range(2):
            (down if i in (0, 1) else up)[t, i].wait_recv()
    for i in (0, 1, 3, 2):
        for t in range(2):
            further[t, i].wait_recv()

    def forward_lin(c):
        (lin_up if c < 2 else lin_down)[c].wait_recv()
        lin_far[c].start()

    phase("inputs")
    h_pair.wait_recv()
    u = jnp.dot(
        hbuf[...].reshape(2 * TOK, 2048), wbuf[...].reshape(2048, 256), preferred_element_type=F32
    ).astype(BF16)
    ubuf[...] = u
    phase("drive")
    forward_lin(0)
    forward_lin(2)
    for j in range(TILES):
        cols = u[:, 128 * (j // 4) : 128 * (j // 4) + 128]
        d = jnp.dot(cols, bh[j], preferred_element_type=F32)
        d += jnp.dot(cols, bl[j], preferred_element_type=F32)
        for s in range(2):
            for k in range(2):
                rows = pl.ds(s * SEQ + (k * TILES + j) * STR, TOK)
                drive[rows, :] = d[TOK * s : TOK * s + TOK, 128 * k : 128 * k + 128]

    def scan(init, keep):
        def body(i, carry):
            carry = list(carry)
            for n in range(8):
                t = i * 8 + n
                for s in range(2):
                    at_re = pl.ds(s * SEQ + t, TILES, stride=STR)
                    at_im = pl.ds(s * SEQ + TILES * STR + t, TILES, stride=STR)
                    re, im = carry[2 * s], carry[2 * s + 1]
                    carry[2 * s] = a_re * re - a_im * im + drive[at_re, :]
                    carry[2 * s + 1] = a_re * im + a_im * re + drive[at_im, :]
                    if keep:
                        drive[at_re, :] = carry[2 * s]
                        drive[at_im, :] = carry[2 * s + 1]
            return tuple(carry)

        return lax.fori_loop(0, TOK // 8, body, init)

    phase("scan1")
    zero = jnp.zeros((8, 128), F32)
    ends = scan((zero,) * 4, False)
    for k in range(4):
        fsend[k] = ends[k]

    def to_later(k):
        return remote(fsend, fbuf.at[sp], fs.at[k], fr.at[sp], (lax.rem(sp + k, 16), dp))

    for k in range(1, 16):

        @pl.when(sp + k < 16)
        def _():
            to_later(k).start()

    phase("pass_l")
    forward_lin(1)
    forward_lin(3)
    for i in range(2):
        for k in (0, 1):
            third[i][k].wait_recv()
            third[i][4 + k].start()
    arrived(lin_up[2:])
    pass_lin(-1)
    arrived(lin_down[:2])
    pass_lin(1)
    for i in range(2):
        arrived(third[i][2:4])
        pass_gate(i, -1)
        pass_gate(i, 1)

    phase("fold")
    def fold(j, carry):
        remote(fsend, fbuf.at[j], fs.at[0], fr.at[j], peer).wait_recv()
        new = []
        for s in range(2):
            re, im = carry[2 * s], carry[2 * s + 1]
            new.append(p_re * re - p_im * im + fbuf[j, 2 * s])
            new.append(p_re * im + p_im * re + fbuf[j, 2 * s + 1])
        return tuple(new)

    begin = lax.fori_loop(0, sp, fold, (zero,) * 4)
    phase("scan2")
    scan(begin, True)
    phase("output")

    for a in range(2):
        tiles = []
        for j in range(4):
            for k in range(2):
                rows = [pl.ds(s * SEQ + (k * TILES + 4 * a + j) * STR, TOK) for s in range(2)]
                tiles.append(jnp.concatenate([drive[r, :] for r in rows], axis=0))
        s_high, s_low = split(jnp.concatenate(tiles, axis=1))
        summed = lax.dot_general(s_high, ch[a], NT, preferred_element_type=F32)
        summed += lax.dot_general(s_low, ch[a], NT, preferred_element_type=F32)
        summed += lax.dot_general(s_high, cl[a], NT, preferred_element_type=F32)
        cols = slice(128 * a, 128 * a + 128)
        mixer = jax.nn.gelu(summed + skv[:, cols] * ubuf[:, cols].astype(F32)).astype(BF16)
        mine = jnp.where(h == 0, mixer[:TOK].astype(F32), mixer[TOK:].astype(F32)).astype(BF16)
        theirs = jnp.where(h == 0, mixer[TOK:].astype(F32), mixer[:TOK].astype(F32)).astype(BF16)
        mbuf[h, :, cols] = mine
        msend[:, cols] = theirs
    m_pair = remote(msend, mbuf.at[h], ms, mr, peer)
    m_pair.start()

    phase("rest_l")
    arrived(lin_far)
    pass_lin(2)
    for i in range(2):
        arrived(third[i][4:])
        pass_gate(i, 2)
    phase("wait_m")
    m_pair.wait_recv()
    for sem in sorted(passed):
        passed[sem].wait_recv()

    m = jnp.concatenate([mbuf[0], mbuf[1]], axis=1)
    phase("project")
    for n in range(8):
        rows = (n // 2, slice(2 * (n % 2), 2 * (n % 2) + 2))
        linear = lax.dot_general(m, lbuf[rows].reshape(256, 512), NT, preferred_element_type=F32)
        gated = lax.dot_general(m, gbuf[rows].reshape(256, 512), NT, preferred_element_type=F32)
        out[0, :, 256 * n : 256 * n + 256] = (linear * jax.nn.sigmoid(gated)).astype(BF16)

    phase("sent")
    for i in range(2):
        for c in first[i] + second[i] + third[i]:
            c.wait_send()
    for c in lin_plane + lin_up + lin_down + lin_far:
        c.wait_send()
    for c in plane + list(up.values()) + list(down.values()) + list(further.values()):
        c.wait_send()
    for sem in sorted(passed):
        passed[sem].wait_send()
    for c in (h_pair, m_pair):
        c.wait_send()
    for k in range(1, 16):

        @pl.when(sp + k < 16)
        def _():
            to_later(k).wait_send()

    phase(None)


def shards(hid, win, lamr, lami, lst, br, bi, cr, ci, skip, lin, gate):
    br, bi = jnp.swapaxes(br, 1, 2), jnp.swapaxes(bi, 1, 2)
    operands = (hid, win, lamr, lami, lst, br, bi, cr, ci, skip.reshape(1, 512), lin.T, gate.T)
    operands = [pltpu.with_memory_space_constraint(a, pltpu.HBM) for a in operands]
    dma = pltpu.SemaphoreType.DMA
    vmem = pltpu.VMEM
    return pl.pallas_call(
        kernel,
        name="mixer",
        out_shape=vmem((1, TOK, 2048), BF16),
        in_specs=[pl.BlockSpec(memory_space=pltpu.HBM)] * 12,
        out_specs=pl.BlockSpec(memory_space=vmem),
        scratch_shapes=[
            vmem((2, TOK, 2048), BF16),
            vmem((4, 4, 4, 2, 16, 256), BF16),
            vmem((4, 4, 4, 2, 16, 512), BF16),
            vmem((4, 4, 4, 2, 16, 512), BF16),
            vmem((2 * SEQ, 128), F32),
            vmem((TILES, 128, 256), BF16),
            vmem((TILES, 128, 256), BF16),
            vmem((2, 128, 1024), BF16),
            vmem((2, 128, 1024), BF16),
            vmem((2 * TOK, 256), BF16),
            vmem((2, GRP, 64), F32),
            pltpu.SMEM((32,), F32),
            vmem((2, GRP, 16, 64), F32),
            vmem((2, GRP, 16, 64), F32),
            vmem((1, 256), F32),
            vmem((16, 256), BF16),
            vmem((2, GRP, 64), F32),
            vmem((16, 4, 8, 128), F32),
            vmem((4, 8, 128), F32),
            vmem((TOK, 256), BF16),
            vmem((2, TOK, 256), BF16),
            dma((13,)),
            dma((4 * PER_ITEM,)),
            dma((4 * PER_ITEM,)),
            dma, dma,
            dma((31,)),
            dma((32,)),
            dma((28,)),
            dma((28,)),
            dma((16,)),
            dma((16,)),
            dma, dma,
            dma((16,)),
            dma((16,)),
        ],
        compiler_params=pltpu.CompilerParams(
            collective_id=0, has_side_effects=True, vmem_limit_bytes=48 * 1024 * 1024
        ),
    )(*operands)


def solution(mesh):
    placed = (
        P("dp", "sp", None),
        P(("sp", "dp"), None),
        *(P(),) * 8,
        P(None, ("sp", "dp")),
        P(None, ("sp", "dp")),
    )
    return jax.shard_map(
        shards, mesh=mesh, in_specs=placed, out_specs=P("dp", "sp", None), check_vma=False
    )
```
